32 devices in a mesh: grp: 2 (over y), ep: 4 (over z), tp: 4 (over x, core).
Axes of the slice: x: 2, y: 2, z: 4, core: 2. Of those that a mesh axis runs over, the one named last changes fastest.
Arguments:
- outer_gate: bfloat16 [4096, 1024], P(('grp', 'ep'), 'tp'), parts along dimension 0, may hold values from -6 to 6
- inner_gate: bfloat16 [4096, 1024], P(('grp', 'ep'), 'tp'), parts along dimension 0, may hold values from -6 to 6
- conv_input: bfloat16 [4096, 1024], P(('grp', 'ep'), 'tp'), parts along dimension 0, may hold values from -6 to 6
- conv_taps: float32 [3, 1024], P(None, 'tp'), may hold values from -3.5 to 3.5
- mixer_weight: bfloat16 [1024, 2048], P('tp'), may hold values from -0.1875 to 0.1875
- expert_input: bfloat16 [4096, 2048], P(('grp', 'ep', 'tp')), parts along dimension 0, may hold values from -6 to 6
- norm_gain: float32 [2048], replicated, may hold values from 0.1 to 1.9
- expert_ids: int32 [4096, 2], P(('grp', 'ep', 'tp')), parts along dimension 0, may hold values from 0 to 3, all different within a row; in each aligned block of 128 rows (0 to 127, 128 to 255, ...) at most 80 rows name the same one
- route_weight: float32 [4096, 2], P(('grp', 'ep', 'tp')), parts along dimension 0, may hold values from 0.25 to 1
- gate_weight: bfloat16 [4, 2048, 3072], P('ep', None, 'tp'), may hold values from -0.125 to 0.125
- up_weight: bfloat16 [4, 2048, 3072], P('ep', None, 'tp'), may hold values from -0.125 to 0.125
- down_weight: bfloat16 [4, 3072, 2048], P('ep', 'tp'), may hold values from -0.109375 to 0.109375
Outputs:
- mixer_output: bfloat16 [4096, 2048], P(('grp', 'ep', 'tp')), parts along dimension 0
- expert_output: bfloat16 [4096, 2048], P(('grp', 'ep', 'tp')), parts along dimension 0
The draws below stay inside these ranges and needn't reach their ends.
There are 2 independent parts, one for each index of `grp`. The reference program is written for one: setup_inputs(seed, part) draws one part's arguments, and reference() takes and returns one part's arrays. A program takes and returns all parts, laid end to end along the dimension named above; an argument that names none is the same for every part. Nothing has to cross between parts.
Inputs may be any that keep to these rules, and one draw needn't show every extreme that they name: `expert_ids`: each row names 2 different experts. Among the rows of one device no expert is named more than 80 times, a bound that some block reaches.
All inputs are finite; a program needn't handle non-finite values.
Results may differ from the reference program's by a relative error of at most 0.011.
Values may be sent and summed in bfloat16 or wider, within the bound.
No kernel may reach another device: no remote copies, remote signals or barrier semaphores. Data moves between devices by JAX's collectives and lax.ppermute only.
A program may use at most 128 MiB of HBM per device.

```python
import math
import jax
import jax.numpy as jnp
import numpy as np
from jax import lax

D = 2048
CONV_W = 1024
TAPS = 3
FF_E = 3072
TOP = 2
TOK_DEV = 128
EXPERTS = 4
CAP = 80
TOKENS = 2048
N_EP = 4
N_TP = 4


def level_of(key, shape, cuts, low, largest):
    gain = 1.0
    for dim, parts in cuts:
        heights = jax.random.uniform(jax.random.fold_in(jax.random.fold_in(key, 6), dim), (parts,), jnp.float32, low / len(cuts), largest / len(cuts))
        gain = gain * jnp.repeat(jnp.exp(heights), shape[dim] // parts).reshape((-1,) + (1,) * (len(shape) - 1 - dim))
    return gain


def deal_out(key, own, number, rows, number_of, top, limit, slope):
    ranking = jax.random.permutation(key, number_of)
    packed, common = shares(number_of, rows * top, limit, slope, True), shares(number_of, rows * top, limit, slope, False)
    places = jnp.arange(number_of)

    def named(lengths, rotation):
        used = int((lengths > 0).sum())
        fixed = max(1, used // 4)
        moved = fixed + (places - fixed + rotation * (used - fixed)) % max(1, number_of - fixed)
        return jnp.zeros((number_of,), jnp.int32).at[ranking[jnp.where(places < fixed, places, moved)]].set(jnp.asarray(lengths, jnp.int32))

    lengths = jnp.where(number % 4 == 0, named(packed, number // 4), named(common, number - number // 4 - 1))
    mixed = jax.random.permutation(jax.random.fold_in(own, 3), number_of)
    source_of, taker = mixed[0:number_of // 2 * 2:2], mixed[1:number_of // 2 * 2:2]
    margin = jnp.minimum(lengths[source_of] - 1, limit - lengths[taker]) // 2
    margin = jnp.where((source_of == ranking[0]) | (taker == ranking[0]) | (lengths[taker] == 0), 0, jnp.maximum(margin, 0))
    moved = jax.random.randint(jax.random.fold_in(own, 4), (number_of // 2,), 0, 1 << 20) % (margin + 1)
    lengths = lengths.at[source_of].add(-moved).at[taker].add(moved)
    members = jnp.searchsorted(jnp.cumsum(lengths), jnp.arange(rows * top), side="right").astype(jnp.int32)
    table = members.reshape(top, rows).T
    table = table[jax.random.permutation(jax.random.fold_in(own, 1), rows)]
    rotation = jax.random.randint(jax.random.fold_in(own, 2), (rows, 1), 0, top)
    return jnp.take_along_axis(table, (jnp.arange(top)[None, :] + rotation) % top, axis=1)


def shares(number_of, total, reach, skew, full):
    portions = [(1 << 20) // math.isqrt(rank ** skew) + 1 for rank in range(1, number_of + 1)]
    largest = reach if full else min(reach, max(-(-total // number_of), total * portions[0] // sum(portions)))
    least = 1 if total - largest >= number_of - 1 else 0
    given, rest = [largest] + [least] * (number_of - 1), total - largest - least * (number_of - 1)
    while rest > 0:
        candidates = [i for i in range(1, number_of) if given[i] < largest] or [i for i in range(1, number_of) if given[i] < reach]
        mass, budget = sum([portions[i] for i in candidates]), rest
        for i in candidates:
            extra = min(reach - given[i], max(1, budget * portions[i] // mass), rest)
            given[i] = given[i] + extra
            rest = rest - extra
    return np.array(given)


def normal_values(stream_key, extent, width, most, split=(), kind=jnp.bfloat16):
    entries = width * jax.random.normal(stream_key, extent, jnp.float32)
    if split:
        entries = entries * level_of(stream_key, extent, split, -0.22, 0.18)
    return jnp.clip(entries, -most, most).astype(kind)


def setup_inputs(seed: int = 0, part: int = 0) -> dict:
    key_of = jax.random.split(jax.random.key(seed), 13)
    part_keys = jax.random.split(jax.random.fold_in(key_of[12], part), 13)
    outer_gate = normal_values(part_keys[0], (TOKENS, CONV_W), 1.0, 6.0, ((0, 4), (1, 4)))
    inner_gate = normal_values(part_keys[1], (TOKENS, CONV_W), 1.0, 6.0, ((0, 4), (1, 4)))
    conv_input = normal_values(part_keys[2], (TOKENS, CONV_W), 1.0, 6.0, ((0, 4), (1, 4)))
    conv_taps = normal_values(key_of[3], (TAPS, CONV_W), TAPS ** -0.5, 3.5, ((1, 4),), jnp.float32)
    mixer_weight = normal_values(key_of[4], (CONV_W, D), CONV_W ** -0.5, 0.1875, ((0, 4),))
    expert_input = normal_values(part_keys[5], (TOKENS, D), 1.0, 6.0, ((0, 16),))
    norm_gain = jnp.clip(1.0 + 0.18 * jax.random.normal(key_of[6], (D,), jnp.float32), 0.1, 1.9)
    expert_ids_keys = jax.random.split(jax.random.fold_in(part_keys[7], 1), TOKENS // TOK_DEV)
    expert_ids_turns = jax.random.permutation(jax.random.fold_in(part_keys[7], 3), TOKENS // TOK_DEV)
    expert_ids = jax.vmap(lambda own, number: deal_out(jax.random.fold_in(part_keys[7], 2), own, number, TOK_DEV, EXPERTS, TOP, CAP, 1))(expert_ids_keys, expert_ids_turns).reshape((TOKENS, TOP))
    route_weight = jnp.clip(jnp.exp(math.log(1.0) - 1.3862944 * jax.random.uniform(part_keys[8], (TOKENS, TOP), jnp.float32) ** level_of(part_keys[8], (TOKENS, TOP), ((0, 16),), -0.2, 0.2)), 0.25, 1.0)
    gate_weight = normal_values(key_of[9], (EXPERTS, D, FF_E), D ** -0.5, 0.125, ((0, 4), (2, 4)))
    up_weight = normal_values(key_of[10], (EXPERTS, D, FF_E), D ** -0.5, 0.125, ((0, 4), (2, 4)))
    down_weight = normal_values(key_of[11], (EXPERTS, FF_E, D), FF_E ** -0.5, 0.109375, ((0, 4), (1, 4)))
    return {"outer_gate": outer_gate, "inner_gate": inner_gate, "conv_input": conv_input, "conv_taps": conv_taps, "mixer_weight": mixer_weight, "expert_input": expert_input, "norm_gain": norm_gain, "expert_ids": expert_ids, "route_weight": route_weight, "gate_weight": gate_weight, "up_weight": up_weight, "down_weight": down_weight}


epsilon = 1e-06

def rounded_sum(operand, weights, pieces):
    slice_width = operand.shape[1] // pieces
    summed = jnp.zeros((operand.shape[0], weights.shape[1]), jnp.float32)
    for piece_index in range(pieces):
        lower = piece_index * slice_width
        partial_value = jnp.dot(operand[:, lower:lower + slice_width], weights[lower:lower + slice_width], preferred_element_type=jnp.float32)
        summed = summed + lax.optimization_barrier(partial_value.astype(jnp.bfloat16)).astype(jnp.float32)
    return summed.astype(jnp.bfloat16)

def reference(outer_gate, inner_gate, conv_input, conv_taps, mixer_weight, expert_input, norm_gain, expert_ids, route_weight, gate_weight, up_weight, down_weight):
    gated_rows = inner_gate.astype(jnp.float32) * conv_input.astype(jnp.float32)
    length = gated_rows.shape[0]
    padded = jnp.pad(gated_rows, ((TAPS - 1, 0), (0, 0)))
    convolved = jnp.zeros_like(gated_rows)
    for tap_index in range(TAPS):
        convolved = convolved + conv_taps[tap_index] * padded[tap_index:tap_index + length]
    mixed = (outer_gate.astype(jnp.float32) * convolved).astype(jnp.bfloat16)
    mixer_output = rounded_sum(mixed, mixer_weight, N_TP)
    inputs = expert_input.astype(jnp.float32)
    normed = (inputs * lax.rsqrt(lax.optimization_barrier(jnp.mean(inputs * inputs, axis=1, keepdims=True)) + epsilon) * norm_gain).astype(jnp.bfloat16)
    flat_ids = expert_ids.reshape(-1)
    flat_weights = route_weight.reshape(-1)
    most_rows = N_EP * N_TP * CAP

    def one_expert(expert):
        chosen = flat_ids == expert
        picked = jnp.nonzero(chosen, size=most_rows, fill_value=0)[0].astype(jnp.int32)
        valid = jnp.arange(most_rows, dtype=jnp.int32) < jnp.sum(chosen.astype(jnp.int32))
        owners = (picked // TOP).astype(jnp.int32)
        token_rows = normed[owners]
        gate_value = jnp.dot(token_rows, gate_weight[expert], preferred_element_type=jnp.float32)
        up_value = jnp.dot(token_rows, up_weight[expert], preferred_element_type=jnp.float32)
        hidden = (jax.nn.silu(gate_value) * up_value).astype(jnp.bfloat16)
        answer = rounded_sum(hidden, down_weight[expert], N_TP)
        pair_weight = jnp.where(valid, flat_weights[picked], jnp.zeros_like(flat_weights[picked]))
        return (owners, answer.astype(jnp.float32) * pair_weight[:, None])
    owners, contributions = lax.map(one_expert, jnp.arange(EXPERTS, dtype=jnp.int32))
    summed = jax.ops.segment_sum(contributions.reshape(-1, D), owners.reshape(-1), num_segments=TOKENS)
    expert_output = summed.astype(jnp.bfloat16)
    return (mixer_output, expert_output)
```

```python
import jax
import jax.numpy as jnp
from jax import lax
from jax.sharding import PartitionSpec as P

TAPS = 3
epsilon = 1e-06
CHUNKS = 4


def swap(value, axis, bit):
    count = lax.axis_size(axis)
    return lax.ppermute(value, axis, [(source, source ^ bit) for source in range(count)])


def high_bits(count):
    bits, bit = [], count // 2
    while bit:
        bits.append(bit)
        bit //= 2
    return bits


def relative_order(count):
    order = [0]
    for bit in high_bits(count):
        order = order + [j ^ bit for j in order]
    return order


def gather_doubling(value, axis):
    for bit in high_bits(lax.axis_size(axis)):
        value = jnp.concatenate([value, swap(value, axis, bit)], axis=0)
    return value


def scatter_halving(value, axis):
    for bit in reversed(high_bits(lax.axis_size(axis))):
        half = value.shape[0] // 2
        received = swap(value[half:].astype(jnp.bfloat16), axis, bit)
        value = value[:half] + received.astype(jnp.float32)
    return value


def on_device(
    outer_gate,
    inner_gate,
    conv_input,
    conv_taps,
    mixer_weight,
    expert_input,
    norm_gain,
    expert_ids,
    route_weight,
    gate_weight,
    up_weight,
    down_weight,
):
    n_ep, n_tp = lax.axis_size("ep"), lax.axis_size("tp")
    tokens_here, top_count = expert_ids.shape
    model_width = expert_input.shape[1]
    expert_count = n_ep * gate_weight.shape[0]
    capacity = 5 * tokens_here * top_count // (4 * expert_count)
    f32, bf16 = jnp.float32, jnp.bfloat16

    inputs = expert_input.astype(f32)
    normed = (
        inputs * lax.rsqrt(jnp.mean(inputs * inputs, axis=1, keepdims=True) + epsilon) * norm_gain
    ).astype(bf16)

    my_ep = lax.axis_index("ep")
    relative = my_ep ^ jnp.arange(n_ep, dtype=jnp.int32)
    ids = expert_ids.T
    chosen = (ids[None] == relative[:, None, None]).astype(f32)
    named = jnp.sum(chosen, axis=1)
    place = jnp.arange(tokens_here, dtype=jnp.int32)
    earlier_token = (place[:, None] < place[None, :]).astype(bf16)
    ranks = jnp.dot(named.astype(bf16), earlier_token, preferred_element_type=f32)
    slots = jnp.arange(capacity, dtype=jnp.int32).astype(f32)
    hit = (ranks[:, None, :] == slots[None, :, None]) & (named[:, None, :] > 0.5)
    select = hit.astype(bf16).reshape(expert_count * capacity, tokens_here)
    outgoing = jnp.dot(select, normed, preferred_element_type=f32).astype(bf16)

    weight_of = jnp.sum(chosen * route_weight.T[None], axis=1)
    spread = jnp.where(hit, weight_of[:, None, :], 0.0).reshape(expert_count * capacity, tokens_here)
    spread_high = spread.astype(bf16)
    spread_low = (spread - spread_high.astype(f32)).astype(bf16)

    blocks = [outgoing[k * capacity : (k + 1) * capacity] for k in range(n_ep)]
    arrived = [blocks[k] if k == 0 else swap(blocks[k], "ep", k) for k in range(n_ep)]

    gated_rows = inner_gate.astype(f32) * conv_input.astype(f32)
    length = gated_rows.shape[0]
    earlier = lax.ppermute(
        gated_rows[length - (TAPS - 1) :], "ep", [(i, i + 1) for i in range(n_ep - 1)]
    )
    padded = jnp.concatenate([earlier, gated_rows], axis=0)
    convolved = jnp.zeros_like(gated_rows)
    for tap_index in range(TAPS):
        convolved = convolved + conv_taps[tap_index] * padded[tap_index : tap_index + length]
    mixed = (outer_gate.astype(f32) * convolved).astype(bf16)
    my_tp = lax.axis_index("tp")
    share = length // n_tp
    mixed = jnp.concatenate(
        [lax.dynamic_slice_in_dim(mixed, (my_tp ^ j) * share, share) for j in relative_order(n_tp)]
    )
    mixer_output = scatter_halving(
        jnp.dot(mixed, mixer_weight, preferred_element_type=f32), "tp"
    ).astype(bf16)

    gate_local, up_local, down_local = gate_weight[0], up_weight[0], down_weight[0]
    group = max(1, n_ep // CHUNKS)
    answers = []
    for first in range(0, n_ep, group):
        rows = gather_doubling(jnp.concatenate(arrived[first : first + group], axis=0), "tp")
        gate_value = jnp.dot(rows, gate_local, preferred_element_type=f32)
        up_value = jnp.dot(rows, up_local, preferred_element_type=f32)
        hidden = (jax.nn.silu(gate_value) * up_value).astype(bf16)
        own = scatter_halving(
            jnp.dot(hidden, down_local, preferred_element_type=f32), "tp"
        ).astype(bf16)
        for k in range(first, first + group):
            part = own[(k - first) * capacity : (k - first + 1) * capacity]
            answers.append(part if k == 0 else swap(part, "ep", k))
    answer = jnp.concatenate(answers, axis=0)
    contract = (((0,), (0,)), ((), ()))
    expert_output = (
        lax.dot_general(spread_high, answer, contract, preferred_element_type=f32)
        + lax.dot_general(spread_low, answer, contract, preferred_element_type=f32)
    ).astype(bf16)
    return (mixer_output, expert_output)


def solution(mesh):
    return jax.shard_map(
        on_device,
        mesh=mesh,
        in_specs=(
            P(("grp", "ep"), "tp"),
            P(("grp", "ep"), "tp"),
            P(("grp", "ep"), "tp"),
            P(None, "tp"),
            P("tp", None),
            P(("grp", "ep", "tp"), None),
            P(),
            P(("grp", "ep", "tp"), None),
            P(("grp", "ep", "tp"), None),
            P("ep", None, "tp"),
            P("ep", None, "tp"),
            P("ep", "tp", None),
        ),
        out_specs=(P(("grp", "ep", "tp"), None), P(("grp", "ep", "tp"), None)),
        check_vma=False,
    )
```
